32 devices in a mesh: sp: 16 (over z, y, x), tp: 2 (over core).
Axes of the slice: x: 2, y: 2, z: 4, core: 2. Of those that a mesh axis runs over, the one named last changes fastest.
Arguments:
- queries: bfloat16 [8192, 1024], P('sp', 'tp'), may hold values from -8 to 8
- key_rows: bfloat16 [8192, 512], P('sp', 'tp'), may hold values from -8 to 8
- values: bfloat16 [8192, 512], P('sp', 'tp'), may hold values from -16 to 16
- doc_ids: int32 [8192], P('sp'), may hold values from 0 to 7, never falling along the last dimension, each value on 1 to 2048 neighbouring positions
- sink_logits: float32 [16], P('tp'), may hold values from 2.5 to 6
- residual: bfloat16 [8192, 2048], P('sp'), may hold values from -6 to 6
- out_weight: bfloat16 [1024, 2048], P('tp'), may hold values from -0.1875 to 0.1875
- norm_gain: float32 [2048], replicated, may hold values from 0.1 to 1.9
- w_gate: bfloat16 [2048, 5632], P('sp', 'tp'), may hold values from -0.125 to 0.125
- w_up: bfloat16 [2048, 5632], P('sp', 'tp'), may hold values from -0.125 to 0.125
- w_down: bfloat16 [5632, 2048], P('tp', 'sp'), may hold values from -0.078125 to 0.078125
Outputs:
- layer_out: bfloat16 [8192, 2048], P('sp')
The draws below stay inside these ranges and needn't reach their ends.
Inputs may be any that keep to these rules, and one draw needn't show every extreme that they name: `doc_ids`: document numbers never fall along the positions; each document has 1 to 2048 positions.
All inputs are finite; a program needn't handle non-finite values.
Results may differ from the reference program's by a relative error of at most 0.014.
Values may be sent and summed in bfloat16 or wider, within the bound.
A program may use at most 128 MiB of HBM per device.

```python
import math
import jax
import jax.numpy as jnp
import numpy as np
from jax import lax

D = 2048
HEADS = 16
KV_HEADS = 8
HD = 64
FF = 5632
WINDOW = 128
TOKENS = 8192
DOCS = 8
DOC_MOST = 2048
N_TP = 2


def drawn_pair(key):
    query_key = jax.random.fold_in(key, 101)
    row_key = jax.random.fold_in(key, 102)
    queries = jnp.clip(jax.random.normal(query_key, (TOKENS, HEADS * HD), jnp.float32), -6.0, 6.0)
    key_rows = jnp.clip(jax.random.normal(row_key, (TOKENS, KV_HEADS * HD), jnp.float32), -6.0, 6.0)
    return (queries, key_rows)


def draw_queries(key, part):
    return drawn_pair(key)[0].astype(jnp.bfloat16)


def draw_key_rows(key, part):
    return drawn_pair(key)[1].astype(jnp.bfloat16)


def steps_of(stream_key, dims, split, low, high):
    loudness, own = 1.0, jax.random.fold_in(stream_key, 6)
    for position, shards_of in split:
        steps = jnp.exp(jax.random.uniform(jax.random.fold_in(own, position), (shards_of,), jnp.float32, low / len(split), high / len(split)))
        loudness = loudness * jnp.repeat(steps, dims[position] // shards_of).reshape([-1 if axis == position else 1 for axis in range(len(dims))])
    return loudness


def split_up(number_of, total, most, skew):
    loads = [(1 << 20) // math.isqrt(grade ** skew) + 1 for grade in range(2, number_of + 1)]
    rest, given = total - most - (number_of - 1), [1] * (number_of - 1)
    while rest > 0:
        candidates = [i for i in range(number_of - 1) if given[i] < most]
        pool, remaining = sum([loads[i] for i in candidates]), rest
        for i in candidates:
            more = min(most - given[i], max(1, remaining * loads[i] // pool), rest)
            given[i] = given[i] + more
            rest = rest - more
    return np.array([most] + given)


def uneven_parts(stream_key, amount, total, reach, slope):
    if amount == 2:
        one = jax.random.randint(stream_key, (), max(1, total - reach), min(reach, total - 1) + 1)
        return jnp.stack([one, total - one])
    lengths = jnp.asarray(split_up(amount, total, reach, slope), jnp.int32)
    couples = (amount - 1) // 2
    source_of, taker = lengths[1:1 + 2 * couples:2], lengths[2:2 + 2 * couples:2]
    room = jnp.minimum(source_of - 1, reach - taker)
    moved = jax.random.randint(jax.random.fold_in(stream_key, 1), (couples,), 0, 1 << 20) % (room + 1)
    lengths = lengths.at[1:1 + 2 * couples:2].set(source_of - moved).at[2:2 + 2 * couples:2].set(taker + moved)
    return lengths[jax.random.permutation(jax.random.fold_in(stream_key, 2), amount)]


def scatter_about(own_key, extent, width, limit, cuts=(), kind=jnp.bfloat16):
    entries = width * jax.random.normal(own_key, extent, jnp.float32)
    if cuts:
        entries = entries * steps_of(own_key, extent, cuts, -0.22, 0.18)
    return jnp.clip(entries, -limit, limit).astype(kind)


def setup_inputs(seed: int = 0) -> dict:
    seeds = jax.random.split(jax.random.key(seed), 12)
    return {
        "queries": draw_queries(jax.random.fold_in(seeds[11], 71), 0),
        "key_rows": draw_key_rows(jax.random.fold_in(seeds[11], 71), 0),
        "values": scatter_about(seeds[2], (TOKENS, KV_HEADS * HD), 3.0, 16.0, ((0, 16), (1, 2))),
        "doc_ids": jnp.searchsorted(jnp.cumsum(uneven_parts(seeds[3], DOCS, TOKENS, DOC_MOST, 1)), jnp.arange(TOKENS), side="right").astype(jnp.int32),
        "sink_logits": jnp.clip(2.5 + 3.5 * jax.random.uniform(seeds[4], (HEADS,), jnp.float32) ** steps_of(seeds[4], (HEADS,), ((0, 2),), -0.2, 0.2), 2.5, 6.0),
        "residual": scatter_about(seeds[5], (TOKENS, D), 1.0, 6.0, ((0, 16),)),
        "out_weight": scatter_about(seeds[6], (HEADS * HD, D), (HEADS * HD) ** -0.5, 0.1875, ((0, 2),)),
        "norm_gain": jnp.clip(1.0 + 0.18 * jax.random.normal(seeds[7], (D,), jnp.float32), 0.1, 1.9),
        "w_gate": scatter_about(seeds[8], (D, FF), D ** -0.5, 0.125, ((0, 16), (1, 2))),
        "w_up": scatter_about(seeds[9], (D, FF), D ** -0.5, 0.125, ((0, 16), (1, 2))),
        "w_down": scatter_about(seeds[10], (FF, D), FF ** -0.5, 0.078125, ((0, 2), (1, 16))),
    }


def rms_norm(stream, norm_gain):
    floats = stream.astype(jnp.float32)
    scale = lax.rsqrt(lax.optimization_barrier(jnp.mean(floats * floats, axis=-1, keepdims=True)) + 1e-06)
    return floats * scale * norm_gain

def band_rows(tensor, blocks):
    tensor = tensor.reshape((blocks + 1, WINDOW) + tensor.shape[1:])
    return jnp.concatenate([tensor[:-1], tensor[1:]], axis=1)

def sliding(queries, key_rows, values, doc_ids, sink_logits):
    total_rows = queries.shape[0]
    blocks = total_rows // WINDOW
    per_kv = HEADS // KV_HEADS
    pad_rows = jnp.zeros((WINDOW, KV_HEADS * HD), jnp.bfloat16)
    key_band = band_rows(jnp.concatenate([pad_rows, key_rows], axis=0), blocks)
    value_band = band_rows(jnp.concatenate([pad_rows, values], axis=0), blocks)
    doc_band = band_rows(jnp.concatenate([jnp.full((WINDOW,), -1, jnp.int32), doc_ids.astype(jnp.int32)]), blocks)
    key_band = key_band.reshape(blocks, 2 * WINDOW, KV_HEADS, HD).astype(jnp.float32)
    value_band = value_band.reshape(blocks, 2 * WINDOW, KV_HEADS, HD).astype(jnp.float32)
    query_band = queries.reshape(blocks, WINDOW, KV_HEADS, per_kv, HD).astype(jnp.float32)
    scores = jnp.einsum('nqhgd,nkhd->nhgqk', query_band, key_band) * HD ** (-0.5)
    offsets = jnp.arange(WINDOW)[:, None] + WINDOW - jnp.arange(2 * WINDOW)[None, :]
    inside = (offsets >= 0) & (offsets < WINDOW)
    query_docs = doc_ids.reshape(blocks, WINDOW)
    allowed = inside[None] & (query_docs[:, :, None] == doc_band[:, None, :])
    scores = jnp.where(allowed[:, None, None], scores, -1e+30)
    sink_logit = sink_logits.reshape(KV_HEADS, per_kv)[None, :, :, None, None]
    peak = jnp.maximum(lax.optimization_barrier(jnp.max(scores, axis=-1, keepdims=True)), sink_logit)
    raised = jnp.exp(scores - peak)
    denom = lax.optimization_barrier(jnp.sum(raised, axis=-1, keepdims=True)) + jnp.exp(sink_logit - peak)
    weights = (raised / denom).astype(jnp.bfloat16)
    attended = jnp.einsum('nhgqk,nkhd->nqhgd', weights.astype(jnp.float32), value_band)
    return attended.astype(jnp.bfloat16).reshape(total_rows, HEADS * HD)

def grouped_sum(left, right, parts):
    columns = left.shape[1] // parts

    def one(carry, index):
        piece = lax.dynamic_slice_in_dim(left, (index * columns).astype(jnp.int32), columns, 1)
        weight = lax.dynamic_slice_in_dim(right, (index * columns).astype(jnp.int32), columns, 0)
        partial_term = jnp.dot(piece, weight, preferred_element_type=jnp.float32).astype(jnp.bfloat16)
        partial_term = lax.optimization_barrier(partial_term)
        return (carry + partial_term.astype(jnp.float32), None)
    start_acc = jnp.zeros((left.shape[0], right.shape[1]), jnp.float32)
    summed, _ = lax.scan(one, start_acc, jnp.arange(parts, dtype=jnp.int32))
    return summed

def feed_forward(normed, w_gate, w_up, w_down, parts):
    columns = w_gate.shape[1] // parts

    def one(carry, index):
        offset = (index * columns).astype(jnp.int32)
        gate_act = jnp.dot(normed, lax.dynamic_slice_in_dim(w_gate, offset, columns, 1), preferred_element_type=jnp.float32)
        up_act = jnp.dot(normed, lax.dynamic_slice_in_dim(w_up, offset, columns, 1), preferred_element_type=jnp.float32)
        hidden = (jax.nn.silu(gate_act) * up_act).astype(jnp.bfloat16)
        weight = lax.dynamic_slice_in_dim(w_down, offset, columns, 0)
        partial_term = jnp.dot(hidden, weight, preferred_element_type=jnp.float32).astype(jnp.bfloat16)
        partial_term = lax.optimization_barrier(partial_term)
        return (carry + partial_term.astype(jnp.float32), None)
    start_acc = jnp.zeros((normed.shape[0], w_down.shape[1]), jnp.float32)
    summed, _ = lax.scan(one, start_acc, jnp.arange(parts, dtype=jnp.int32))
    return summed

def reference(queries, key_rows, values, doc_ids, sink_logits, residual, out_weight, norm_gain, w_gate, w_up, w_down):
    attended = sliding(queries, key_rows, values, doc_ids, sink_logits)
    mixed_sum = grouped_sum(attended, out_weight, N_TP)
    stream = (residual.astype(jnp.float32) + mixed_sum).astype(jnp.bfloat16)
    normed = rms_norm(stream, norm_gain).astype(jnp.bfloat16)
    mlp_total = feed_forward(normed, w_gate, w_up, w_down, N_TP)
    return (stream.astype(jnp.float32) + mlp_total).astype(jnp.bfloat16)
```

```python
import jax
import jax.numpy as jnp
from jax import lax
from jax.sharding import PartitionSpec as P

HD = 64
WINDOW = 128
INNER = 4


def from_behind(shard, axis, by):
    size = lax.axis_size(axis)
    pairs = [(i, i + by) for i in range(size) if 0 <= i + by < size]
    return lax.ppermute(shard, axis, pairs)


def rms_norm(stream, norm_gain):
    floats = stream.astype(jnp.float32)
    scale = lax.rsqrt(jnp.mean(floats * floats, axis=-1, keepdims=True) + 1e-06)
    return floats * scale * norm_gain


def band_rows(tensor, blocks):
    tensor = tensor.reshape((blocks + 1, WINDOW) + tensor.shape[1:])
    return jnp.concatenate([tensor[:-1], tensor[1:]], axis=1)


def attend(queries, key_rows, values, doc_ids, sink_logits):
    local_rows = queries.shape[0]
    blocks = local_rows // WINDOW
    kv_local = key_rows.shape[1] // HD
    per_kv = queries.shape[1] // key_rows.shape[1]
    tail_docs = doc_ids[local_rows - WINDOW :] + 1
    prev_keys, prev_values, prev_docs = from_behind(
        (key_rows[local_rows - WINDOW :], values[local_rows - WINDOW :], tail_docs), "sp", 1
    )
    key_band = band_rows(jnp.concatenate([prev_keys, key_rows], axis=0), blocks).reshape(
        blocks, 2 * WINDOW, kv_local, HD
    )
    value_band = band_rows(jnp.concatenate([prev_values, values], axis=0), blocks).reshape(
        blocks, 2 * WINDOW, kv_local, HD
    )
    doc_band = band_rows(jnp.concatenate([prev_docs - 1, doc_ids]), blocks)
    query_band = queries.reshape(blocks, WINDOW, kv_local, per_kv, HD)
    scores = jnp.einsum(
        "nqhgd,nkhd->nhgqk", query_band, key_band, preferred_element_type=jnp.float32
    ) * HD ** (-0.5)
    offsets = jnp.arange(WINDOW)[:, None] + WINDOW - jnp.arange(2 * WINDOW)[None, :]
    inside = (offsets >= 0) & (offsets < WINDOW)
    query_docs = doc_ids.reshape(blocks, WINDOW)
    allowed = inside[None] & (query_docs[:, :, None] == doc_band[:, None, :])
    scores = jnp.where(allowed[:, None, None], scores, -1e30)
    sink_logit = sink_logits.reshape(kv_local, per_kv)[None, :, :, None, None]
    peak = jnp.maximum(jnp.max(scores, axis=-1, keepdims=True), sink_logit)
    raised = jnp.exp(scores - peak)
    denom = jnp.sum(raised, axis=-1, keepdims=True) + jnp.exp(sink_logit - peak)
    weights = (raised / denom).astype(jnp.bfloat16)
    attended = jnp.einsum(
        "nhgqk,nkhd->nqhgd", weights, value_band, preferred_element_type=jnp.float32
    )
    return attended.astype(jnp.bfloat16).reshape(local_rows, queries.shape[1])


def swap(shard, axis, by):
    size = lax.axis_size(axis)
    return lax.ppermute(shard, axis, [(i, i ^ by) for i in range(size)])


def piece_of(tensor, index, axis, pieces):
    size = tensor.shape[axis] // pieces
    return lax.dynamic_slice_in_dim(tensor, index * size, size, axis)


def in_order(mine, others, place, axis):
    size = mine.shape[axis]
    shape = list(mine.shape)
    shape[axis] = size * (len(others) + 1)
    whole = jnp.zeros(shape, mine.dtype)
    for k, shard in enumerate([mine] + others):
        whole = lax.dynamic_update_slice_in_dim(whole, shard, (place ^ k) * size, axis)
    return whole


def on_device(
    queries,
    key_rows,
    values,
    doc_ids,
    sink_logits,
    residual,
    out_weight,
    norm_gain,
    w_gate,
    w_up,
    w_down,
):
    inner = INNER
    outer = lax.axis_size("sp") // inner
    tp = lax.axis_size("tp")
    seat = lax.rem(lax.axis_index("sp"), inner)
    core = lax.axis_index("tp")
    columns = [[row + inner * step for step in range(outer)] for row in range(inner)]

    def gate_up_piece(k):
        return jnp.concatenate(
            [piece_of(w_gate, seat ^ k, 1, inner), piece_of(w_up, seat ^ k, 1, inner)], axis=1
        )

    gate_up = in_order(
        gate_up_piece(0), [swap(gate_up_piece(k), "sp", k) for k in range(1, inner)], seat, 0
    )
    gate_up = lax.all_gather(gate_up, "sp", axis=0, tiled=True, axis_index_groups=columns)
    down = in_order(
        piece_of(w_down, seat, 0, inner)[None],
        [swap(piece_of(w_down, seat ^ k, 0, inner), "sp", k)[None] for k in range(1, inner)],
        seat,
        0,
    )
    down = lax.all_gather(down, "sp", axis=0, tiled=True, axis_index_groups=columns)
    down = jnp.swapaxes(down, 0, 1).reshape(down.shape[1], -1)

    attended = attend(queries, key_rows, values, doc_ids, sink_logits)
    mix_term = jnp.dot(attended, out_weight, preferred_element_type=jnp.float32).astype(jnp.bfloat16)
    mixed_sum = piece_of(mix_term, core, 0, tp).astype(jnp.float32)
    for k in range(1, tp):
        mixed_sum += swap(piece_of(mix_term, core ^ k, 0, tp), "tp", k).astype(jnp.float32)
    stream = (piece_of(residual, core, 0, tp).astype(jnp.float32) + mixed_sum).astype(jnp.bfloat16)
    normed = rms_norm(stream, norm_gain).astype(jnp.bfloat16)
    rows, width = normed.shape
    near = jnp.concatenate([normed] + [swap(normed, "sp", k) for k in range(1, inner)], axis=0)
    tokens = jnp.concatenate([near] + [swap(near, "tp", k) for k in range(1, tp)], axis=0)

    acts = jnp.dot(tokens, gate_up, preferred_element_type=jnp.float32)
    units = acts.shape[1] // 2
    hidden = (jax.nn.silu(acts[:, :units]) * acts[:, units:]).astype(jnp.bfloat16)
    mlp_term = jnp.dot(hidden, down, preferred_element_type=jnp.float32).astype(jnp.bfloat16)
    mlp_term = mlp_term.reshape(tp, inner * rows, width)
    near_sum = mlp_term[0].astype(jnp.float32)
    for k in range(1, tp):
        near_sum += swap(mlp_term[k], "tp", k).astype(jnp.float32)
    near_sum = near_sum.reshape(inner, rows, width)
    total = near_sum[0]
    for k in range(1, inner):
        total += swap(near_sum[k].astype(jnp.bfloat16), "sp", k).astype(jnp.float32)
    out = (stream.astype(jnp.float32) + total).astype(jnp.bfloat16)
    return in_order(out, [swap(out, "tp", k) for k in range(1, tp)], core, 0)


def solution(mesh):
    in_specs = (
        P("sp", "tp"),
        P("sp", "tp"),
        P("sp", "tp"),
        P("sp"),
        P("tp"),
        P("sp", None),
        P("tp", None),
        P(),
        P("sp", "tp"),
        P("sp", "tp"),
        P("tp", "sp"),
    )
    out_specs = P("sp", None)
    return jax.shard_map(
        on_device, mesh=mesh, in_specs=in_specs, out_specs=out_specs, check_vma=False
    )
```

```python
import jax
import jax.numpy as jnp
from jax import lax
from jax.sharding import PartitionSpec as P

HD = 64
WINDOW = 128
INNER = 4
CHUNKS = 2


def from_behind(shard, axis, by):
    size = lax.axis_size(axis)
    pairs = [(i, i + by) for i in range(size) if 0 <= i + by < size]
    return lax.ppermute(shard, axis, pairs)


def rms_norm(stream, norm_gain):
    floats = stream.astype(jnp.float32)
    scale = lax.rsqrt(jnp.mean(floats * floats, axis=-1, keepdims=True) + 1e-06)
    return floats * scale * norm_gain


def band_rows(tensor, blocks):
    tensor = tensor.reshape((blocks + 1, WINDOW) + tensor.shape[1:])
    return jnp.concatenate([tensor[:-1], tensor[1:]], axis=1)


def attend(queries, key_rows, values, doc_ids, sink_logits):
    local_rows = queries.shape[0]
    blocks = local_rows // WINDOW
    kv_local = key_rows.shape[1] // HD
    per_kv = queries.shape[1] // key_rows.shape[1]
    tail_docs = doc_ids[local_rows - WINDOW :] + 1
    width = key_rows.shape[1]
    tail = jnp.concatenate(
        [
            key_rows[local_rows - WINDOW :],
            values[local_rows - WINDOW :],
            jnp.broadcast_to(tail_docs.astype(jnp.bfloat16)[:, None], (WINDOW, 128)),
        ],
        axis=1,
    )
    tail = from_behind(tail, "sp", 1)
    prev_keys, prev_values = tail[:, :width], tail[:, width : 2 * width]
    prev_docs = tail[:, 2 * width].astype(jnp.int32)
    key_band = band_rows(jnp.concatenate([prev_keys, key_rows], axis=0), blocks).reshape(
        blocks, 2 * WINDOW, kv_local, HD
    )
    value_band = band_rows(jnp.concatenate([prev_values, values], axis=0), blocks).reshape(
        blocks, 2 * WINDOW, kv_local, HD
    )
    doc_band = band_rows(jnp.concatenate([prev_docs - 1, doc_ids]), blocks)
    query_band = queries.reshape(blocks, WINDOW, kv_local, per_kv, HD)
    scores = jnp.einsum(
        "nqhgd,nkhd->nhgqk", query_band, key_band, preferred_element_type=jnp.float32
    ) * HD ** (-0.5)
    offsets = jnp.arange(WINDOW)[:, None] + WINDOW - jnp.arange(2 * WINDOW)[None, :]
    inside = (offsets >= 0) & (offsets < WINDOW)
    query_docs = doc_ids.reshape(blocks, WINDOW)
    allowed = inside[None] & (query_docs[:, :, None] == doc_band[:, None, :])
    scores = jnp.where(allowed[:, None, None], scores, -1e30)
    sink_logit = sink_logits.reshape(kv_local, per_kv)[None, :, :, None, None]
    peak = jnp.maximum(jnp.max(scores, axis=-1, keepdims=True), sink_logit)
    raised = jnp.exp(scores - peak)
    denom = jnp.sum(raised, axis=-1, keepdims=True) + jnp.exp(sink_logit - peak)
    weights = (raised / denom).astype(jnp.bfloat16)
    attended = jnp.einsum(
        "nhgqk,nkhd->nqhgd", weights, value_band, preferred_element_type=jnp.float32
    )
    return attended.astype(jnp.bfloat16).reshape(local_rows, queries.shape[1])


def swap(shard, axis, by):
    size = lax.axis_size(axis)
    return lax.ppermute(shard, axis, [(i, i ^ by) for i in range(size)])


def piece_of(tensor, index, axis, pieces):
    size = tensor.shape[axis] // pieces
    return lax.dynamic_slice_in_dim(tensor, index * size, size, axis)


def in_order(mine, others, place, axis):
    size = mine.shape[axis]
    shape = list(mine.shape)
    shape[axis] = size * (len(others) + 1)
    whole = jnp.zeros(shape, mine.dtype)
    for k, shard in enumerate([mine] + others):
        whole = lax.dynamic_update_slice_in_dim(whole, shard, (place ^ k) * size, axis)
    return whole


def on_device(
    queries,
    key_rows,
    values,
    doc_ids,
    sink_logits,
    residual,
    out_weight,
    norm_gain,
    w_gate,
    w_up,
    w_down,
):
    inner = INNER
    outer = lax.axis_size("sp") // inner
    tp = lax.axis_size("tp")
    seat = lax.rem(lax.axis_index("sp"), inner)
    core = lax.axis_index("tp")
    columns = [[row + inner * step for step in range(outer)] for row in range(inner)]

    def gate_up_piece(k):
        return jnp.concatenate(
            [piece_of(w_gate, seat ^ k, 1, inner), piece_of(w_up, seat ^ k, 1, inner)], axis=1
        )

    def down_piece(k):
        return piece_of(w_down, seat ^ k, 0, inner)[None]

    gate_up_pieces = [gate_up_piece(k) for k in range(inner)]
    down_pieces = [down_piece(k) for k in range(inner)]
    gate_up_pieces, down_pieces, queries, key_rows, values = lax.optimization_barrier(
        (gate_up_pieces, down_pieces, queries, key_rows, values)
    )
    down = in_order(
        down_pieces[0], [swap(down_pieces[k], "sp", k) for k in range(1, inner)], seat, 0
    )
    gate_up = in_order(
        gate_up_pieces[0], [swap(gate_up_pieces[k], "sp", k) for k in range(1, inner)], seat, 0
    )

    def across(block):
        return lax.all_gather(block, "sp", axis=0, tiled=True, axis_index_groups=columns)

    def flat(gathered):
        return jnp.swapaxes(gathered, 0, 1).reshape(gathered.shape[1], -1)

    part = inner // CHUNKS
    downs = [across(down[:part])]
    gate_up = across(gate_up)
    downs += [across(down[c * part : (c + 1) * part]) for c in range(1, CHUNKS)]

    attended = attend(queries, key_rows, values, doc_ids, sink_logits)
    mix_term = jnp.dot(attended, out_weight, preferred_element_type=jnp.float32).astype(jnp.bfloat16)
    mixed_sum = piece_of(mix_term, core, 0, tp).astype(jnp.float32)
    for k in range(1, tp):
        mixed_sum += swap(piece_of(mix_term, core ^ k, 0, tp), "tp", k).astype(jnp.float32)
    stream = (piece_of(residual, core, 0, tp).astype(jnp.float32) + mixed_sum).astype(jnp.bfloat16)
    normed = rms_norm(stream, norm_gain).astype(jnp.bfloat16)
    rows, width = normed.shape
    near = jnp.concatenate([normed] + [swap(normed, "sp", k) for k in range(1, inner)], axis=0)
    tokens = jnp.concatenate([near] + [swap(near, "tp", k) for k in range(1, tp)], axis=0)

    acts = jnp.dot(tokens, gate_up, preferred_element_type=jnp.float32)
    units = acts.shape[1] // 2
    hidden = (jax.nn.silu(acts[:, :units]) * acts[:, units:]).astype(jnp.bfloat16)
    block = width // (outer * CHUNKS)
    outs = []
    for c in range(CHUNKS):
        mlp_term = jnp.dot(hidden, lax.optimization_barrier(flat(downs[c])), preferred_element_type=jnp.float32)
        mlp_term = mlp_term.astype(jnp.bfloat16).reshape(tp, inner * rows, width // CHUNKS)
        near_sum = mlp_term[0].astype(jnp.float32)
        for k in range(1, tp):
            near_sum += swap(mlp_term[k], "tp", k).astype(jnp.float32)
        near_sum = near_sum.reshape(inner, rows, width // CHUNKS)
        total = near_sum[0]
        for k in range(1, inner):
            total += swap(near_sum[k].astype(jnp.bfloat16), "sp", k).astype(jnp.float32)
        outs.append(total)
    total = jnp.concatenate(
        [outs[c][:, o * block : (o + 1) * block] for o in range(outer) for c in range(CHUNKS)],
        axis=1,
    )
    out = (stream.astype(jnp.float32) + total).astype(jnp.bfloat16)
    return in_order(out, [swap(out, "tp", k) for k in range(1, tp)], core, 0)


def solution(mesh):
    in_specs = (
        P("sp", "tp"),
        P("sp", "tp"),
        P("sp", "tp"),
        P("sp"),
        P("tp"),
        P("sp", None),
        P("tp", None),
        P(),
        P("sp", "tp"),
        P("sp", "tp"),
        P("tp", "sp"),
    )
    out_specs = P("sp", None)
    return jax.shard_map(
        on_device, mesh=mesh, in_specs=in_specs, out_specs=out_specs, check_vma=False
    )
```

```python
import jax
import jax.numpy as jnp
from jax import lax
from jax.sharding import PartitionSpec as P


HD = 64
WINDOW = 128
INNER = 4
CHUNKS = 2


def from_behind(shard, axis, by):
    size = lax.axis_size(axis)
    pairs = [(i, i + by) for i in range(size) if 0 <= i + by < size]
    return lax.ppermute(shard, axis, pairs)


def rms_norm(stream, norm_gain):
    floats = stream.astype(jnp.float32)
    scale = lax.rsqrt(jnp.mean(floats * floats, axis=-1, keepdims=True) + 1e-06)
    return floats * scale * norm_gain


def band_rows(tensor, blocks):
    tensor = tensor.reshape((blocks + 1, WINDOW) + tensor.shape[1:])
    return jnp.concatenate([tensor[:-1], tensor[1:]], axis=1)


def attend(queries, key_rows, values, doc_ids, sink_logits):
    local_rows = queries.shape[0]
    blocks = local_rows // WINDOW
    kv_local = key_rows.shape[1] // HD
    per_kv = queries.shape[1] // key_rows.shape[1]
    tail_docs = doc_ids[local_rows - WINDOW :] + 1
    width = key_rows.shape[1]
    tail = jnp.concatenate(
        [
            key_rows[local_rows - WINDOW :],
            values[local_rows - WINDOW :],
            jnp.broadcast_to(tail_docs.astype(jnp.bfloat16)[:, None], (WINDOW, 128)),
        ],
        axis=1,
    )
    tail = from_behind(tail, "sp", 1)
    prev_keys, prev_values = tail[:, :width], tail[:, width : 2 * width]
    prev_docs = tail[:, 2 * width].astype(jnp.int32)
    key_band = band_rows(jnp.concatenate([prev_keys, key_rows], axis=0), blocks).reshape(
        blocks, 2 * WINDOW, kv_local, HD
    )
    value_band = band_rows(jnp.concatenate([prev_values, values], axis=0), blocks).reshape(
        blocks, 2 * WINDOW, kv_local, HD
    )
    doc_band = band_rows(jnp.concatenate([prev_docs - 1, doc_ids]), blocks)
    query_band = queries.reshape(blocks, WINDOW, kv_local, per_kv, HD)
    scores = jnp.einsum(
        "nqhgd,nkhd->nhgqk", query_band, key_band, preferred_element_type=jnp.float32
    ) * HD ** (-0.5)
    offsets = jnp.arange(WINDOW)[:, None] + WINDOW - jnp.arange(2 * WINDOW)[None, :]
    inside = (offsets >= 0) & (offsets < WINDOW)
    query_docs = doc_ids.reshape(blocks, WINDOW)
    allowed = inside[None] & (query_docs[:, :, None] == doc_band[:, None, :])
    scores = jnp.where(allowed[:, None, None], scores, -1e30)
    sink_logit = sink_logits.reshape(kv_local, per_kv)[None, :, :, None, None]
    peak = jnp.maximum(jnp.max(scores, axis=-1, keepdims=True), sink_logit)
    raised = jnp.exp(scores - peak)
    denom = jnp.sum(raised, axis=-1, keepdims=True) + jnp.exp(sink_logit - peak)
    weights = (raised / denom).astype(jnp.bfloat16)
    attended = jnp.einsum(
        "nhgqk,nkhd->nqhgd", weights, value_band, preferred_element_type=jnp.float32
    )
    return attended.astype(jnp.bfloat16).reshape(local_rows, queries.shape[1])


def swap(shard, axis, by):
    size = lax.axis_size(axis)
    return lax.ppermute(shard, axis, [(i, i ^ by) for i in range(size)])


def piece_of(tensor, index, axis, pieces):
    size = tensor.shape[axis] // pieces
    return lax.dynamic_slice_in_dim(tensor, index * size, size, axis)


def in_order(mine, others, place, axis):
    size = mine.shape[axis]
    shape = list(mine.shape)
    shape[axis] = size * (len(others) + 1)
    whole = jnp.zeros(shape, mine.dtype)
    for k, shard in enumerate([mine] + others):
        whole = lax.dynamic_update_slice_in_dim(whole, shard, (place ^ k) * size, axis)
    return whole


def on_device(
    queries,
    key_rows,
    values,
    doc_ids,
    sink_logits,
    residual,
    out_weight,
    norm_gain,
    w_gate,
    w_up,
    w_down,
):
    inner = INNER
    outer = lax.axis_size("sp") // inner
    tp = lax.axis_size("tp")
    seat = lax.rem(lax.axis_index("sp"), inner)
    core = lax.axis_index("tp")
    columns = [[row + inner * step for step in range(outer)] for row in range(inner)]

    def gate_up_piece(k):
        return jnp.concatenate(
            [piece_of(w_gate, seat ^ k, 1, inner), piece_of(w_up, seat ^ k, 1, inner)], axis=1
        )

    def down_piece(k):
        return piece_of(w_down, seat ^ k, 0, inner)[None]

    gate_up_pieces = [gate_up_piece(k) for k in range(inner)]
    gate_up_pieces, queries, key_rows, values, w_down = lax.optimization_barrier(
        (gate_up_pieces, queries, key_rows, values, w_down)
    )
    gate_up = in_order(
        gate_up_pieces[0], [swap(gate_up_pieces[k], "sp", k) for k in range(1, inner)], seat, 0
    )
    down = in_order(
        down_piece(0), [swap(down_piece(k), "sp", k) for k in range(1, inner)], seat, 0
    )

    def across(block):
        return lax.all_gather(block, "sp", axis=0, tiled=True, axis_index_groups=columns)

    def flat(gathered):
        return jnp.swapaxes(gathered, 0, 1).reshape(gathered.shape[1], -1)

    part = inner // CHUNKS
    gate_up = across(gate_up)
    downs = []
    for c in range(CHUNKS):
        downs.append(across(down[c * part : (c + 1) * part]))

    attended = attend(queries, key_rows, values, doc_ids, sink_logits)
    mix_term = jnp.dot(attended, out_weight, preferred_element_type=jnp.float32).astype(jnp.bfloat16)
    mixed_sum = piece_of(mix_term, core, 0, tp).astype(jnp.float32)
    for k in range(1, tp):
        mixed_sum += swap(piece_of(mix_term, core ^ k, 0, tp), "tp", k).astype(jnp.float32)
    stream = (piece_of(residual, core, 0, tp).astype(jnp.float32) + mixed_sum).astype(jnp.bfloat16)
    normed = rms_norm(stream, norm_gain).astype(jnp.bfloat16)
    rows, width = normed.shape
    near = jnp.concatenate([normed] + [swap(normed, "sp", k) for k in range(1, inner)], axis=0)
    tokens = jnp.concatenate([near] + [swap(near, "tp", k) for k in range(1, tp)], axis=0)

    acts = jnp.dot(tokens, gate_up, preferred_element_type=jnp.float32)
    units = acts.shape[1] // 2
    hidden = (jax.nn.silu(acts[:, :units]) * acts[:, units:]).astype(jnp.bfloat16)
    block = width // (outer * CHUNKS)
    outs = []
    for c in range(CHUNKS):
        mlp_term = jnp.dot(hidden, lax.optimization_barrier(flat(downs[c])), preferred_element_type=jnp.float32)
        mlp_term = mlp_term.astype(jnp.bfloat16).reshape(tp, inner * rows, width // CHUNKS)
        near_sum = mlp_term[0].astype(jnp.float32)
        for k in range(1, tp):
            near_sum += swap(mlp_term[k], "tp", k).astype(jnp.float32)
        near_sum = near_sum.reshape(inner, rows, width // CHUNKS)
        sends = [near_sum[k].astype(jnp.bfloat16) for k in range(1, inner)]
        total = near_sum[0]
        for k in range(1, inner):
            sent = swap(sends[k - 1], "sp", k)
            total += sent.astype(jnp.float32)
        outs.append(total)
    total = jnp.concatenate(
        [outs[c][:, o * block : (o + 1) * block] for o in range(outer) for c in range(CHUNKS)],
        axis=1,
    )
    out = (stream.astype(jnp.float32) + total).astype(jnp.bfloat16)
    return in_order(out, [swap(out, "tp", k) for k in range(1, tp)], core, 0)


def solution(mesh):
    in_specs = (
        P("sp", "tp"),
        P("sp", "tp"),
        P("sp", "tp"),
        P("sp"),
        P("tp"),
        P("sp", None),
        P("tp", None),
        P(),
        P("sp", "tp"),
        P("sp", "tp"),
        P("tp", "sp"),
    )
    out_specs = P("sp", None)

    return jax.shard_map(
        on_device, mesh=mesh, in_specs=in_specs, out_specs=out_specs, check_vma=False
    )
```

```python
import jax
import jax.numpy as jnp
from jax import lax
from jax.sharding import PartitionSpec as P


HD = 64
WINDOW = 128
INNER = 4
CHUNKS = 2


def from_behind(shard, axis, by):
    size = lax.axis_size(axis)
    pairs = [(i, i + by) for i in range(size) if 0 <= i + by < size]
    return lax.ppermute(shard, axis, pairs)


def rms_norm(stream, norm_gain):
    floats = stream.astype(jnp.float32)
    scale = lax.rsqrt(jnp.mean(floats * floats, axis=-1, keepdims=True) + 1e-06)
    return floats * scale * norm_gain


def band_rows(tensor, blocks):
    tensor = tensor.reshape((blocks + 1, WINDOW) + tensor.shape[1:])
    return jnp.concatenate([tensor[:-1], tensor[1:]], axis=1)


def attend(queries, key_rows, values, doc_ids, sink_logits):
    local_rows = queries.shape[0]
    blocks = local_rows // WINDOW
    kv_local = key_rows.shape[1] // HD
    per_kv = queries.shape[1] // key_rows.shape[1]
    tail_docs = doc_ids[local_rows - WINDOW :] + 1
    width = key_rows.shape[1]
    tail = jnp.concatenate(
        [
            key_rows[local_rows - WINDOW :],
            values[local_rows - WINDOW :],
            jnp.broadcast_to(tail_docs.astype(jnp.bfloat16)[:, None], (WINDOW, 128)),
        ],
        axis=1,
    )
    tail = from_behind(tail, "sp", 1)
    prev_keys, prev_values = tail[:, :width], tail[:, width : 2 * width]
    prev_docs = tail[:, 2 * width].astype(jnp.int32)
    key_band = band_rows(jnp.concatenate([prev_keys, key_rows], axis=0), blocks).reshape(
        blocks, 2 * WINDOW, kv_local, HD
    )
    value_band = band_rows(jnp.concatenate([prev_values, values], axis=0), blocks).reshape(
        blocks, 2 * WINDOW, kv_local, HD
    )
    doc_band = band_rows(jnp.concatenate([prev_docs - 1, doc_ids]), blocks)
    query_band = queries.reshape(blocks, WINDOW, kv_local, per_kv, HD)
    scores = jnp.einsum(
        "nqhgd,nkhd->nhgqk", query_band, key_band, preferred_element_type=jnp.float32
    ) * HD ** (-0.5)
    offsets = jnp.arange(WINDOW)[:, None] + WINDOW - jnp.arange(2 * WINDOW)[None, :]
    inside = (offsets >= 0) & (offsets < WINDOW)
    query_docs = doc_ids.reshape(blocks, WINDOW)
    allowed = inside[None] & (query_docs[:, :, None] == doc_band[:, None, :])
    scores = jnp.where(allowed[:, None, None], scores, -1e30)
    sink_logit = sink_logits.reshape(kv_local, per_kv)[None, :, :, None, None]
    peak = jnp.maximum(jnp.max(scores, axis=-1, keepdims=True), sink_logit)
    raised = jnp.exp(scores - peak)
    denom = jnp.sum(raised, axis=-1, keepdims=True) + jnp.exp(sink_logit - peak)
    weights = (raised / denom).astype(jnp.bfloat16)
    attended = jnp.einsum(
        "nhgqk,nkhd->nqhgd", weights, value_band, preferred_element_type=jnp.float32
    )
    return attended.astype(jnp.bfloat16).reshape(local_rows, queries.shape[1])


def swap(shard, axis, by):
    size = lax.axis_size(axis)
    return lax.ppermute(shard, axis, [(i, i ^ by) for i in range(size)])


def piece_of(tensor, index, axis, pieces):
    size = tensor.shape[axis] // pieces
    return lax.dynamic_slice_in_dim(tensor, index * size, size, axis)


def in_order(mine, others, place, axis):
    size = mine.shape[axis]
    shape = list(mine.shape)
    shape[axis] = size * (len(others) + 1)
    whole = jnp.zeros(shape, mine.dtype)
    for k, shard in enumerate([mine] + others):
        whole = lax.dynamic_update_slice_in_dim(whole, shard, (place ^ k) * size, axis)
    return whole


def on_device(
    queries,
    key_rows,
    values,
    doc_ids,
    sink_logits,
    residual,
    out_weight,
    norm_gain,
    w_gate,
    w_up,
    w_down,
):
    inner = INNER
    outer = lax.axis_size("sp") // inner
    tp = lax.axis_size("tp")
    seat = lax.rem(lax.axis_index("sp"), inner)
    core = lax.axis_index("tp")
    columns = [[row + inner * step for step in range(outer)] for row in range(inner)]

    def gate_up_piece(k):
        return jnp.concatenate(
            [piece_of(w_gate, seat ^ k, 1, inner), piece_of(w_up, seat ^ k, 1, inner)], axis=1
        )

    def down_piece(k):
        return piece_of(w_down, seat ^ k, 0, inner)[None]

    gate_up_pieces = [gate_up_piece(k) for k in range(inner)]
    _, queries, key_rows, values, w_down = lax.optimization_barrier(
        (gate_up_pieces[1:], queries, key_rows, values, w_down)
    )
    gate_up = in_order(
        gate_up_pieces[0], [swap(gate_up_pieces[k], "sp", k) for k in range(1, inner)], seat, 0
    )
    down = in_order(
        down_piece(0), [swap(down_piece(k), "sp", k) for k in range(1, inner)], seat, 0
    )

    def across(block):
        return lax.all_gather(block, "sp", axis=0, tiled=True, axis_index_groups=columns)

    def flat(gathered):
        return jnp.swapaxes(gathered, 0, 1).reshape(gathered.shape[1], -1)

    part = inner // CHUNKS
    gate_up = across(gate_up)
    downs = []
    for c in range(CHUNKS):
        downs.append(across(down[c * part : (c + 1) * part]))

    attended = attend(queries, key_rows, values, doc_ids, sink_logits)
    mix_term = jnp.dot(attended, out_weight, preferred_element_type=jnp.float32).astype(jnp.bfloat16)
    mixed_sum = piece_of(mix_term, core, 0, tp).astype(jnp.float32)
    for k in range(1, tp):
        mixed_sum += swap(piece_of(mix_term, core ^ k, 0, tp), "tp", k).astype(jnp.float32)
    stream = (piece_of(residual, core, 0, tp).astype(jnp.float32) + mixed_sum).astype(jnp.bfloat16)
    normed = rms_norm(stream, norm_gain).astype(jnp.bfloat16)
    rows, width = normed.shape
    near = jnp.concatenate([normed] + [swap(normed, "sp", k) for k in range(1, inner)], axis=0)
    tokens = jnp.concatenate([near] + [swap(near, "tp", k) for k in range(1, tp)], axis=0)

    acts = jnp.dot(tokens, gate_up, preferred_element_type=jnp.float32)
    units = acts.shape[1] // 2
    hidden = (jax.nn.silu(acts[:, :units]) * acts[:, units:]).astype(jnp.bfloat16)
    block = width // (outer * CHUNKS)
    outs = []
    for c in range(CHUNKS):
        mlp_term = jnp.dot(hidden, lax.optimization_barrier(flat(downs[c])), preferred_element_type=jnp.float32)
        mlp_term = mlp_term.astype(jnp.bfloat16).reshape(tp, inner * rows, width // CHUNKS)
        near_sum = mlp_term[0].astype(jnp.float32)
        for k in range(1, tp):
            near_sum += swap(mlp_term[k], "tp", k).astype(jnp.float32)
        near_sum = near_sum.reshape(inner, rows, width // CHUNKS)
        sends = [near_sum[k].astype(jnp.bfloat16) for k in range(1, inner)]
        total = near_sum[0]
        for k in range(1, inner):
            sent = swap(sends[k - 1], "sp", k)
            total += sent.astype(jnp.float32)
        mine = jnp.concatenate(
            [
                stream[:, (o * CHUNKS + c) * block : (o * CHUNKS + c + 1) * block]
                for o in range(outer)
            ],
            axis=1,
        )
        mine = (mine.astype(jnp.float32) + total).astype(jnp.bfloat16)
        outs.append(in_order(mine, [swap(mine, "tp", k) for k in range(1, tp)], core, 0))
    return jnp.concatenate(
        [outs[c][:, o * block : (o + 1) * block] for o in range(outer) for c in range(CHUNKS)],
        axis=1,
    )


def solution(mesh):
    in_specs = (
        P("sp", "tp"),
        P("sp", "tp"),
        P("sp", "tp"),
        P("sp"),
        P("tp"),
        P("sp", None),
        P("tp", None),
        P(),
        P("sp", "tp"),
        P("sp", "tp"),
        P("tp", "sp"),
    )
    out_specs = P("sp", None)

    return jax.shard_map(
        on_device, mesh=mesh, in_specs=in_specs, out_specs=out_specs, check_vma=False
    )
```
